32 devices in a mesh: sp: 16 (over z, y, x), tp: 2 (over core).
Axes of the slice: x: 2, y: 2, z: 4, core: 2. Of those that a mesh axis runs over, the one named last changes fastest.
Arguments:
- queries: bfloat16 [8192, 2048], P('sp', 'tp'), may hold values from -6 to 6
- keys: bfloat16 [8192, 1024], P('sp', 'tp'), may hold values from -6 to 6
- values: bfloat16 [8192, 1024], P('sp', 'tp'), may hold values from -6 to 6
- documents: int32 [8192], P('sp'), may hold values from 0 to 3, never falling along the last dimension, each value on 1 to 4096 neighbouring positions
- query_gain: float32 [128], replicated, may hold values from 1.8 to 6
- key_gain: float32 [128], replicated, may hold values from 1.8 to 6
- residual: bfloat16 [8192, 4096], P('sp', 'tp'), may hold values from -6 to 6
- out_weight: bfloat16 [2048, 4096], P('tp'), may hold values from -0.125 to 0.125
- norm_gain: float32 [4096], replicated, may hold values from 0.1 to 1.9
- up_weight: bfloat16 [4096, 16384], P('sp', 'tp'), may hold values from -0.09375 to 0.09375
- down_weight: bfloat16 [16384, 4096], P('tp', 'sp'), may hold values from -0.046875 to 0.046875
Outputs:
- mixed: bfloat16 [8192, 4096], P('sp', 'tp')
The draws below stay inside these ranges and needn't reach their ends.
Inputs may be any that keep to these rules, and one draw needn't show every extreme that they name: `documents`: document numbers never fall along the sequence; a document has at most 4096 positions.
All inputs are finite; a program needn't handle non-finite values.
Results may differ from the reference program's by a relative error of at most 0.017.
The reference program's roundings to bfloat16 on the way count: a program that leaves them out, or rounds other values in their place, can miss the bound.
Values may be sent and summed in bfloat16 or wider, within the bound.
No kernel may reach another device: no remote copies, remote signals or barrier semaphores. Data moves between devices by JAX's collectives and lax.ppermute only.
A program may use at most 256 MiB of HBM per device.

```python
import math
import jax
import jax.numpy as jnp
import numpy as np
from jax import lax

D = 4096
FF = 16384
HQ = 16
KV = 8
HD = 128
GRID_W = 64
TOK_DEV = 512
TOKENS = 8192
DOCS = 4
DOC_MOST = 4096
N_SP = 16
N_TP = 2


def drawn_keys(key):
    base = jnp.clip(jax.random.normal(jax.random.fold_in(key, 11), (TOKENS, KV * HD), jnp.float32), -6.0, 6.0)
    return base


def draw_keys(key, part):
    return drawn_keys(key).astype(jnp.bfloat16)


def draw_queries(key, part):
    base = jnp.clip(jax.random.normal(jax.random.fold_in(key, 12), (TOKENS, HQ * HD), jnp.float32), -6.0, 6.0)
    return base.astype(jnp.bfloat16)


def gain_values(key, offset):
    return jax.random.uniform(jax.random.fold_in(key, offset), (HD,), jnp.float32, 1.8, 3.0)


def draw_query_gain(key, part):
    return gain_values(key, 21)


def draw_key_gain(key, part):
    return gain_values(key, 22)


def steps_of(rng, dims, cuts, smallest, top_value):
    def one(axis_at, blocks):
        steps = jax.random.uniform(jax.random.fold_in(jax.random.fold_in(rng, 6), axis_at), (blocks,), jnp.float32, smallest / len(cuts), top_value / len(cuts))
        return jnp.repeat(jnp.exp(steps), dims[axis_at] // blocks).reshape((-1,) + (1,) * (len(dims) - axis_at - 1))

    level = one(*cuts[0])
    for cut in cuts[1:]:
        level = level * one(*cut)
    return level


def split_up(count, total, bound, skew):
    loads = [(1 << 20) // math.isqrt(rank ** skew) + 1 for rank in range(2, count + 1)]
    rest, counts = total - bound - (count - 1), [1] * (count - 1)
    while rest > 0:
        movable = [i for i in range(count - 1) if counts[i] < bound]
        pool, remaining = sum([loads[i] for i in movable]), rest
        for i in movable:
            extra = min(bound - counts[i], max(1, remaining * loads[i] // pool), rest)
            counts[i] = counts[i] + extra
            rest = rest - extra
    return np.array([bound] + counts)


def ragged_sizes(own_key, amount, total, bound, slope):
    if amount == 2:
        one = jax.random.randint(own_key, (), max(1, total - bound), min(bound, total - 1) + 1)
        return jnp.stack([one, total - one])
    sizes = jnp.asarray(split_up(amount, total, bound, slope), jnp.int32)
    couples = (amount - 1) // 2
    giver, receiver = sizes[1:1 + 2 * couples:2], sizes[2:2 + 2 * couples:2]
    margin = jnp.minimum(giver - 1, bound - receiver)
    passed = jax.random.randint(jax.random.fold_in(own_key, 1), (couples,), 0, 1 << 20) % (margin + 1)
    sizes = sizes.at[1:1 + 2 * couples:2].set(giver - passed).at[2:2 + 2 * couples:2].set(receiver + passed)
    return sizes[jax.random.permutation(jax.random.fold_in(own_key, 2), amount)]


def scatter_about(own_key, shape, spread, bound, split=(), kind=jnp.bfloat16):
    level = steps_of(own_key, shape, split, -0.22, 0.18) if split else 1.0
    values = jax.random.normal(own_key, shape, jnp.float32) * spread * level
    return jnp.minimum(jnp.maximum(values, -bound), bound).astype(kind)


def setup_inputs(seed: int = 0) -> dict:
    seeds = jax.random.split(jax.random.key(seed), 12)
    return {
        "queries": draw_queries(jax.random.fold_in(seeds[11], 71), 0),
        "keys": draw_keys(jax.random.fold_in(seeds[11], 71), 0),
        "values": scatter_about(seeds[2], (TOKENS, KV * HD), 1.0, 6.0, ((0, 16), (1, 2))),
        "documents": jnp.searchsorted(jnp.cumsum(ragged_sizes(seeds[3], DOCS, TOKENS, DOC_MOST, 0)), jnp.arange(TOKENS), side="right").astype(jnp.int32),
        "query_gain": draw_query_gain(jax.random.fold_in(seeds[11], 71), 0),
        "key_gain": draw_key_gain(jax.random.fold_in(seeds[11], 71), 0),
        "residual": scatter_about(seeds[6], (TOKENS, D), 1.0, 6.0, ((0, 16), (1, 2))),
        "out_weight": scatter_about(seeds[7], (HQ * HD, D), (HQ * HD) ** -0.5, 0.125, ((0, 2),)),
        "norm_gain": jnp.clip(1.0 + 0.18 * jax.random.normal(seeds[8], (D,), jnp.float32), 0.1, 1.9),
        "up_weight": scatter_about(seeds[9], (D, FF), D ** -0.5, 0.09375, ((0, 16), (1, 2))),
        "down_weight": scatter_about(seeds[10], (FF, D), FF ** -0.5, 0.046875, ((0, 2), (1, 16))),
    }


norm_eps = 1e-06
rope_base = 10000.0
masked_score = -1e+30

def head_norm(heads_in, gain):
    values32 = heads_in.astype(jnp.float32)
    scaled = values32 * lax.rsqrt(lax.optimization_barrier(jnp.mean(values32 * values32, axis=-1, keepdims=True)) + norm_eps)
    return scaled * gain.astype(jnp.float32)

def rotate_half(heads_in, position):
    quarter = heads_in.shape[-1] // 2
    inverse_freq = rope_base ** (-jnp.arange(quarter, dtype=jnp.float32) / quarter)
    angles = position[:, None] * inverse_freq[None, :]
    cosine_part = jnp.cos(angles)[:, None, :]
    sine_part = jnp.sin(angles)[:, None, :]
    leading = heads_in[..., :quarter]
    trailing = heads_in[..., quarter:]
    return jnp.concatenate([leading * cosine_part - trailing * sine_part, leading * sine_part + trailing * cosine_part], axis=-1)

def grid_rotary(heads_in, positions):
    half_width = heads_in.shape[-1] // 2
    grid_row = (positions // GRID_W).astype(jnp.float32)
    grid_col = (positions % GRID_W).astype(jnp.float32)
    return jnp.concatenate([rotate_half(heads_in[..., :half_width], grid_row), rotate_half(heads_in[..., half_width:], grid_col)], axis=-1)

def reference(queries, keys, values, documents, query_gain, key_gain, residual, out_weight, norm_gain, up_weight, down_weight):
    group_size = HQ // KV
    positions = jnp.arange(TOKENS, dtype=jnp.int32)
    queries_rot = grid_rotary(head_norm(queries.reshape(TOKENS, HQ, HD), query_gain), positions).astype(jnp.bfloat16)
    keys_rot = grid_rotary(head_norm(keys.reshape(TOKENS, KV, HD), key_gain), positions).astype(jnp.bfloat16)
    key_float = keys_rot.astype(jnp.float32)
    value_float = values.reshape(TOKENS, KV, HD).astype(jnp.float32)
    query_blocks = queries_rot.reshape(N_SP, TOK_DEV, KV, group_size, HD)
    doc_blocks = documents.reshape(N_SP, TOK_DEV)

    def attend(block_pair):
        query_block, doc_block = block_pair
        scores = jnp.einsum('qkgd,skd->kgqs', query_block.astype(jnp.float32), key_float) * HD ** (-0.5)
        same_doc = doc_block[:, None] == documents[None, :]
        scores = jnp.where(same_doc, scores, masked_score)
        row_max = lax.optimization_barrier(jnp.max(scores, axis=-1, keepdims=True))
        probs = jnp.where(same_doc, jnp.exp(scores - row_max), 0.0)
        row_sum = lax.optimization_barrier(jnp.sum(probs, axis=-1))
        probs_low = lax.optimization_barrier(probs.astype(jnp.bfloat16)).astype(jnp.float32)
        summed = jnp.einsum('kgqs,skd->qkgd', probs_low, value_float)
        return (summed / jnp.transpose(row_sum, (2, 0, 1))[..., None]).astype(jnp.bfloat16)
    attended = lax.map(attend, (query_blocks, doc_blocks)).reshape(TOKENS, HQ * HD)
    head_width = HQ * HD // N_TP
    branch = jnp.zeros((TOKENS, D), jnp.float32)
    for head_block in range(N_TP):
        lower = head_block * head_width
        part_sum = jnp.dot(attended[:, lower:lower + head_width], out_weight[lower:lower + head_width], preferred_element_type=jnp.float32)
        branch = branch + lax.optimization_barrier(part_sum.astype(jnp.bfloat16)).astype(jnp.float32)
    stream = residual.astype(jnp.float32) + branch
    normed = stream * lax.rsqrt(lax.optimization_barrier(jnp.mean(stream * stream, axis=-1, keepdims=True)) + norm_eps)
    normed = (normed * norm_gain.astype(jnp.float32)).astype(jnp.bfloat16)
    hidden = jnp.dot(normed, up_weight, preferred_element_type=jnp.float32)
    positive = jnp.maximum(hidden, 0.0)
    squared = (positive * positive).astype(jnp.bfloat16)
    unit_width = FF // N_TP
    feed = jnp.zeros((TOKENS, D), jnp.float32)
    for unit_block in range(N_TP):
        lower = unit_block * unit_width
        part_sum = jnp.dot(squared[:, lower:lower + unit_width], down_weight[lower:lower + unit_width], preferred_element_type=jnp.float32)
        feed = feed + lax.optimization_barrier(part_sum.astype(jnp.bfloat16)).astype(jnp.float32)
    return (stream + feed).astype(jnp.bfloat16)
```

```python
import functools
import jax
import jax.numpy as jnp
from jax import lax
from jax.experimental import pallas as pl
from jax.experimental.pallas import tpu as pltpu
from jax.sharding import PartitionSpec as P


HQ = 16
KV = 8
HD = 128
GRID_W = 64

norm_eps = 1e-06
rope_base = 10000.0
masked_score = -1e30
log2_e = 1.4426950408889634


def head_norm(heads_in, gain):
    values32 = heads_in.astype(jnp.float32)
    scaled = values32 * lax.rsqrt(jnp.mean(values32 * values32, axis=-1, keepdims=True) + norm_eps)
    return scaled * gain


def rotate_half(heads_in, position):
    quarter = heads_in.shape[-1] // 2
    inverse_freq = rope_base ** (-jnp.arange(quarter, dtype=jnp.float32) / quarter)
    angles = position[:, None] * inverse_freq[None, :]
    cosine_part = jnp.cos(angles)[:, None, :]
    sine_part = jnp.sin(angles)[:, None, :]
    leading = heads_in[..., :quarter]
    trailing = heads_in[..., quarter:]
    return jnp.concatenate(
        [
            leading * cosine_part - trailing * sine_part,
            leading * sine_part + trailing * cosine_part,
        ],
        axis=-1,
    )


def grid_rotary(heads_in, positions):
    half_width = heads_in.shape[-1] // 2
    grid_row = (positions // GRID_W).astype(jnp.float32)
    grid_col = (positions % GRID_W).astype(jnp.float32)
    return jnp.concatenate(
        [
            rotate_half(heads_in[..., :half_width], grid_row),
            rotate_half(heads_in[..., half_width:], grid_col),
        ],
        axis=-1,
    )


def attend_kernel(flags, q_ref, kv_ref, qdoc_ref, kdoc_ref, out_ref, max_ref, sum_ref, acc_ref, *, group, blocks):
    tile = pl.program_id(0)
    tokens = q_ref.shape[0]
    factor = log2_e * HD ** (-0.5)
    rows = jnp.concatenate([q_ref[:, g * HD : (g + 1) * HD] for g in range(group)], axis=0)
    max_ref[...] = jnp.full(max_ref.shape, masked_score, jnp.float32)
    sum_ref[...] = jnp.zeros(sum_ref.shape, jnp.float32)
    acc_ref[...] = jnp.zeros(acc_ref.shape, jnp.float32)

    def block_step(block, masked):
        scores = lax.dot_general(
            kv_ref[block, :, :HD], rows, (((1,), (1,)), ((), ())), preferred_element_type=jnp.float32
        )
        if masked:
            same = kdoc_ref[block] == qdoc_ref[0]
            scores = jnp.where(same, scores, masked_score)
        old_max = max_ref[...]
        new_max = jnp.maximum(old_max, jnp.max(scores, axis=0, keepdims=True))
        alpha = jnp.exp2((old_max - new_max) * factor)
        probs = jnp.exp2((scores - new_max) * factor)
        if masked:
            probs = jnp.where(same, probs, 0.0)
        sum_ref[...] = sum_ref[...] * alpha + jnp.sum(probs, axis=0, keepdims=True)
        acc_ref[...] = acc_ref[...] * alpha + lax.dot_general(
            kv_ref[block, :, HD:],
            probs.astype(jnp.bfloat16),
            (((0,), (0,)), ((), ())),
            preferred_element_type=jnp.float32,
        )
        max_ref[...] = new_max

    def loop_body(block, carry):
        kind = flags[tile * blocks + block]

        @pl.when(kind == 1)
        def _():
            block_step(block, True)

        @pl.when(kind == 2)
        def _():
            block_step(block, False)

        return carry

    lax.fori_loop(0, blocks, loop_body, 0)
    result = jnp.transpose(acc_ref[...] / sum_ref[...]).astype(jnp.bfloat16)
    for g in range(group):
        out_ref[:, g * HD : (g + 1) * HD] = result[g * tokens : (g + 1) * tokens]


def attend(q_blocks, kv_blocks, q_docs, kv_docs, group):
    q_count, rows, width = q_blocks.shape
    blocks, block_rows, _ = kv_blocks.shape
    tile_rows = min(256, rows)
    tiles = q_count * rows // tile_rows
    q_flat = q_blocks.reshape(tiles * tile_rows, width)
    q_tiles = q_docs.reshape(tiles, tile_rows)
    low, high = q_tiles[:, :1], q_tiles[:, -1:]
    key_low, key_high = kv_docs[None, :, 0], kv_docs[None, :, -1]
    needed = (key_low <= high) & (key_high >= low)
    whole = (low == high) & (key_low == key_high)
    flags = jnp.where(needed, jnp.where(whole, 2, 1), 0).astype(jnp.int32).reshape(-1)
    grid_spec = pltpu.PrefetchScalarGridSpec(
        num_scalar_prefetch=1,
        grid=(tiles,),
        in_specs=[
            pl.BlockSpec((tile_rows, width), lambda t, f: (t, 0)),
            pl.BlockSpec((blocks, block_rows, 2 * HD), lambda t, f: (0, 0, 0)),
            pl.BlockSpec((1, 1, group * tile_rows), lambda t, f: (t, 0, 0)),
            pl.BlockSpec((blocks, block_rows, 1), lambda t, f: (0, 0, 0)),
        ],
        out_specs=pl.BlockSpec((tile_rows, width), lambda t, f: (t, 0)),
        scratch_shapes=[
            pltpu.VMEM((1, group * tile_rows), jnp.float32),
            pltpu.VMEM((1, group * tile_rows), jnp.float32),
            pltpu.VMEM((HD, group * tile_rows), jnp.float32),
        ],
    )
    pairs = tiles * tile_rows * group * blocks * block_rows
    out = pl.pallas_call(
        functools.partial(attend_kernel, group=group, blocks=blocks),
        grid_spec=grid_spec,
        out_shape=jax.ShapeDtypeStruct(q_flat.shape, jnp.bfloat16),
        cost_estimate=pl.CostEstimate(
            flops=2 * pairs * HD, bytes_accessed=4 * q_flat.size + 2 * kv_blocks.size, transcendentals=pairs // 2
        ),
        name="attend",
    )(flags, q_flat, kv_blocks, jnp.tile(q_tiles, (1, group))[:, None, :], kv_docs[:, :, None])
    return out.reshape(q_blocks.shape)


def up_kernel(part, col, *refs, tp, slots, slab):
    x_refs, w_ref, out_ref, rows_ref = refs[:tp], refs[tp], refs[tp + 1], refs[tp + 2]

    @pl.when(pl.program_id(0) == 0)
    def _():
        for s in range(slots):
            for j in range(tp):

                @pl.when(part[s] == j)
                def _(s=s, j=j):
                    at = pl.multiple_of(col[s], slab)
                    rows_ref[:, s * slab : (s + 1) * slab] = x_refs[j][:, pl.ds(at, slab)]

    hidden = jnp.dot(rows_ref[...], w_ref[...], preferred_element_type=jnp.float32)
    positive = jnp.maximum(hidden, 0.0)
    out_ref[...] = (positive * positive).astype(jnp.bfloat16)


def up_project(part, col, parts, weight, slots):
    tp = len(parts)
    rows, width = parts[0].shape
    depth, units = weight.shape
    block = min(256, units)
    grid_spec = pltpu.PrefetchScalarGridSpec(
        num_scalar_prefetch=2,
        grid=(units // block,),
        in_specs=[pl.BlockSpec((rows, width), lambda n, a, b: (0, 0))] * tp
        + [pl.BlockSpec((depth, block), lambda n, a, b: (0, n))],
        out_specs=pl.BlockSpec((rows, block), lambda n, a, b: (0, n)),
        scratch_shapes=[pltpu.VMEM((rows, depth), jnp.bfloat16)],
    )
    return pl.pallas_call(
        functools.partial(up_kernel, tp=tp, slots=slots, slab=depth // slots),
        grid_spec=grid_spec,
        out_shape=jax.ShapeDtypeStruct((rows, units), jnp.bfloat16),
        cost_estimate=pl.CostEstimate(
            flops=2 * rows * depth * units, bytes_accessed=2 * depth * (units + rows), transcendentals=0
        ),
    )(part, col, *parts, weight)


def down_kernel(part, col, x_ref, w_ref, *out_refs, slab):
    s = pl.program_id(0)
    result = jnp.dot(x_ref[...], w_ref[...], preferred_element_type=jnp.float32).astype(jnp.bfloat16)
    for j, out_ref in enumerate(out_refs):

        @pl.when(part[s] == j)
        def _(out_ref=out_ref):
            out_ref[:, pl.ds(pl.multiple_of(col[s], slab), slab)] = result


def down_project(part, col, squared, weight, tp, slots):
    rows, units = squared.shape
    slab = weight.shape[1]
    width = slab * slots // tp
    grid_spec = pltpu.PrefetchScalarGridSpec(
        num_scalar_prefetch=2,
        grid=(slots,),
        in_specs=[
            pl.BlockSpec((rows, units), lambda s, a, b: (0, 0)),
            pl.BlockSpec((units, slab), lambda s, a, b: (s, 0)),
        ],
        out_specs=[pl.BlockSpec((rows, width), lambda s, a, b: (0, 0))] * tp,
    )
    return pl.pallas_call(
        functools.partial(down_kernel, slab=slab),
        grid_spec=grid_spec,
        out_shape=[jax.ShapeDtypeStruct((rows, width), jnp.bfloat16)] * tp,
        cost_estimate=pl.CostEstimate(
            flops=2 * rows * units * slab * slots, bytes_accessed=2 * units * (slab * slots + rows), transcendentals=0
        ),
    )(part, col, squared, weight)


def make_body(outer, inner, tp):
    def swap_outer(value, k):
        pairs = [(o * inner + i, (o ^ k) * inner + i) for o in range(outer) for i in range(inner)]
        return lax.ppermute(value, "sp", pairs)

    def swap_inner(value, r):
        pairs = [(o * inner + i, o * inner + (i ^ r)) for o in range(outer) for i in range(inner)]
        return lax.ppermute(value, "sp", pairs)

    def swap_tp(value, j):
        return lax.ppermute(value, "tp", [(t, t ^ j) for t in range(tp)])

    def gather_inner(value):
        if inner != 4:
            return [value] + [swap_inner(value, r) for r in range(1, inner)]
        half = value.shape[0] // 2
        first, second = swap_inner(value, 1), swap_inner(value, 2)
        corner_a = swap_inner(second[:half], 1)
        corner_b = swap_inner(first[half:], 2)
        return [value, first, second, corner_a, corner_b]

    def body(
        queries, keys, values, documents, query_gain, key_gain, residual, out_weight, norm_gain, up_weight, down_weight
    ):
        rows = queries.shape[0]
        key_heads = keys.shape[1] // HD
        group = HQ // KV
        width = residual.shape[1]
        sp_index = lax.axis_index("sp")
        o, i, t = sp_index // inner, sp_index % inner, lax.axis_index("tp")
        split = key_heads % outer == 0
        units = up_weight.shape[1] // outer
        slab = up_weight.shape[0]
        far = range(1, outer)
        places = [(r, k) for r in range(inner) for k in (0,)] + [(r, k) for r in range(inner) for k in far]
        slots = len(places)
        spots = jnp.stack([((o ^ k) * inner + (i ^ r)) * slab for r, k in places]).astype(jnp.int32)
        part = (spots // width) ^ t.astype(jnp.int32)
        col = spots % width

        docs_outer = jnp.stack([documents] + [swap_outer(documents, k) for k in far])
        docs_all = jnp.concatenate([docs_outer] + [swap_inner(docs_outer, r) for r in range(1, inner)])

        up_near = gather_inner(lax.dynamic_slice_in_dim(up_weight, o * units, units, 1))
        down_near = gather_inner(lax.dynamic_slice_in_dim(down_weight, o * units, units, 0))
        up_pieces = [swap_outer(lax.dynamic_slice_in_dim(up_weight, (o ^ k) * units, units, 1), k) for k in far]
        down_pieces = [swap_outer(lax.dynamic_slice_in_dim(down_weight, (o ^ k) * units, units, 0), k) for k in far]
        up_far = gather_inner(jnp.concatenate(up_pieces))
        down_far = gather_inner(jnp.concatenate(down_pieces))

        positions = sp_index * rows + jnp.arange(rows, dtype=jnp.int32)
        queries_rot = grid_rotary(
            head_norm(queries.reshape(rows, key_heads * group, HD), query_gain), positions
        ).astype(jnp.bfloat16)
        keys_rot = grid_rotary(head_norm(keys.reshape(rows, key_heads, HD), key_gain), positions).astype(jnp.bfloat16)
        parts = outer if split else 1
        heads = key_heads // parts
        q_width = heads * group * HD
        packed = jnp.concatenate(
            [
                queries_rot.reshape(rows, parts, q_width),
                keys_rot.reshape(rows, parts, heads * HD),
                values.reshape(rows, parts, heads * HD),
            ],
            axis=-1,
        )
        packed = jnp.transpose(packed, (1, 0, 2))
        if split:
            taken = [lax.dynamic_index_in_dim(packed, o ^ k, 0, keepdims=False) for k in range(outer)]
            taken = [taken[0]] + [swap_outer(taken[k], k) for k in far]
            q_blocks = jnp.stack([piece[:, :q_width] for piece in taken])
            kv_own = jnp.concatenate([piece[:, q_width:] for piece in taken])
            q_docs = docs_outer
        else:
            q_blocks = packed[:, :, :q_width]
            kv_mine = packed[0, :, q_width:]
            kv_own = jnp.concatenate([kv_mine] + [swap_outer(kv_mine, k) for k in far])
            q_docs = documents[None]
        kv_all = jnp.concatenate(gather_inner(kv_own)).reshape(outer * inner, rows, -1)

        attended = []
        for h in range(heads):
            q_head = q_blocks[:, :, h * group * HD : (h + 1) * group * HD]
            kv_head = kv_all
            if heads > 1:
                kv_head = jnp.concatenate(
                    [kv_all[:, :, h * HD : (h + 1) * HD], kv_all[:, :, (heads + h) * HD : (heads + h + 1) * HD]], -1
                )
            attended.append(attend(q_head, kv_head, q_docs, docs_all, group))
        attended = attended[0] if heads == 1 else jnp.concatenate(attended, -1)
        if split:
            merged = jnp.zeros((rows, outer * q_width), jnp.bfloat16)
            for k in range(outer):
                piece = attended[k] if k == 0 else swap_outer(attended[k], k)
                merged = lax.dynamic_update_slice_in_dim(merged, piece, (o ^ k) * q_width, 1)
            attended = merged
        else:
            attended = attended[0]

        partial_out = jnp.dot(attended, out_weight, preferred_element_type=jnp.float32).astype(jnp.bfloat16)
        stream = residual.astype(jnp.float32)
        for j in range(tp):
            piece = lax.dynamic_slice_in_dim(partial_out, (t ^ j) * width, width, 1)
            piece = piece if j == 0 else swap_tp(piece, j)
            stream = stream + piece.astype(jnp.float32)
        squares = jnp.sum(stream * stream, axis=-1)
        total_squares = squares
        for j in range(1, tp):
            total_squares = total_squares + swap_tp(squares, j)
        gain_here = lax.dynamic_slice_in_dim(norm_gain, t * width, width, 0)
        normed = stream * lax.rsqrt(total_squares / (width * tp) + norm_eps)[:, None]
        normed = (normed * gain_here).astype(jnp.bfloat16)

        up_whole = jnp.concatenate(up_near + up_far)
        down_whole = jnp.concatenate(down_near + down_far)

        squared = []
        for k in range(outer):
            chunk = normed if k == 0 else swap_outer(normed, k)
            chunk_parts = [chunk]
            for j in range(1, tp):
                chunk_parts.append(swap_tp(chunk, j))
            squared.append(up_project(part, col, chunk_parts, up_whole, slots))
        feed = [None] * outer
        for k in list(far)[::-1] + [0]:
            pieces = down_project(part, col, squared[k], down_whole, tp, slots)
            total = pieces[0].astype(jnp.float32)
            for j in range(1, tp):
                total = total + swap_tp(pieces[j], j).astype(jnp.float32)
            feed[k] = total if k == 0 else swap_outer(total.astype(jnp.bfloat16), k)
        result = stream
        for k in range(outer):
            result = result + feed[k].astype(jnp.float32)
        return result.astype(jnp.bfloat16)

    return body


def solution(mesh):
    sp, tp = mesh.shape["sp"], mesh.shape["tp"]
    outer = 1 << (sp.bit_length() // 2)
    inner = sp // outer
    in_specs = (
        P("sp", "tp"),
        P("sp", "tp"),
        P("sp", "tp"),
        P("sp"),
        P(),
        P(),
        P("sp", "tp"),
        P("tp", None),
        P(),
        P("sp", "tp"),
        P("tp", "sp"),
    )
    return jax.shard_map(
        make_body(outer, inner, tp), mesh=mesh, in_specs=in_specs, out_specs=P("sp", "tp"), check_vma=False
    )
```

```python
import functools
import jax
import jax.numpy as jnp
from jax import lax
from jax.experimental import pallas as pl
from jax.experimental.pallas import tpu as pltpu
from jax.sharding import PartitionSpec as P


HQ = 16
KV = 8
HD = 128
GRID_W = 64

norm_eps = 1e-06
rope_base = 10000.0
masked_score = -1e30
log2_e = 1.4426950408889634


def head_norm(heads_in, gain):
    values32 = heads_in.astype(jnp.float32)
    scaled = values32 * lax.rsqrt(jnp.mean(values32 * values32, axis=-1, keepdims=True) + norm_eps)
    return scaled * gain


def rotate_half(heads_in, position):
    quarter = heads_in.shape[-1] // 2
    inverse_freq = rope_base ** (-jnp.arange(quarter, dtype=jnp.float32) / quarter)
    angles = position[:, None] * inverse_freq[None, :]
    cosine_part = jnp.cos(angles)[:, None, :]
    sine_part = jnp.sin(angles)[:, None, :]
    leading = heads_in[..., :quarter]
    trailing = heads_in[..., quarter:]
    return jnp.concatenate(
        [
            leading * cosine_part - trailing * sine_part,
            leading * sine_part + trailing * cosine_part,
        ],
        axis=-1,
    )


def grid_rotary(heads_in, positions):
    half_width = heads_in.shape[-1] // 2
    grid_row = (positions // GRID_W).astype(jnp.float32)
    grid_col = (positions % GRID_W).astype(jnp.float32)
    return jnp.concatenate(
        [
            rotate_half(heads_in[..., :half_width], grid_row),
            rotate_half(heads_in[..., half_width:], grid_col),
        ],
        axis=-1,
    )


def attend_kernel(flags, q_ref, kv_ref, qdoc_ref, kdoc_ref, out_ref, max_ref, sum_ref, acc_ref, *, group, blocks):
    tile = pl.program_id(0)
    tokens = q_ref.shape[0]
    factor = log2_e * HD ** (-0.5)
    rows = jnp.concatenate([q_ref[:, g * HD : (g + 1) * HD] for g in range(group)], axis=0)
    max_ref[...] = jnp.full(max_ref.shape, masked_score, jnp.float32)
    sum_ref[...] = jnp.zeros(sum_ref.shape, jnp.float32)
    acc_ref[...] = jnp.zeros(acc_ref.shape, jnp.float32)

    def block_step(block, masked):
        scores = lax.dot_general(
            kv_ref[block, :, :HD], rows, (((1,), (1,)), ((), ())), preferred_element_type=jnp.float32
        )
        if masked:
            same = kdoc_ref[block] == qdoc_ref[0]
            scores = jnp.where(same, scores, masked_score)
        old_max = max_ref[...]
        new_max = jnp.maximum(old_max, jnp.max(scores, axis=0, keepdims=True))
        alpha = jnp.exp2((old_max - new_max) * factor)
        probs = jnp.exp2((scores - new_max) * factor)
        if masked:
            probs = jnp.where(same, probs, 0.0)
        sum_ref[...] = sum_ref[...] * alpha + jnp.sum(probs, axis=0, keepdims=True)
        acc_ref[...] = acc_ref[...] * alpha + lax.dot_general(
            kv_ref[block, :, HD:],
            probs.astype(jnp.bfloat16),
            (((0,), (0,)), ((), ())),
            preferred_element_type=jnp.float32,
        )
        max_ref[...] = new_max

    def loop_body(block, carry):
        kind = flags[tile * blocks + block]

        @pl.when(kind == 1)
        def _():
            block_step(block, True)

        @pl.when(kind == 2)
        def _():
            block_step(block, False)

        return carry

    lax.fori_loop(0, blocks, loop_body, 0)
    result = jnp.transpose(acc_ref[...] / sum_ref[...]).astype(jnp.bfloat16)
    for g in range(group):
        out_ref[:, g * HD : (g + 1) * HD] = result[g * tokens : (g + 1) * tokens]


def attend(q_blocks, kv_blocks, q_docs, kv_docs, group):
    q_count, rows, width = q_blocks.shape
    blocks, block_rows, _ = kv_blocks.shape
    tile_rows = min(256, rows)
    tiles = q_count * rows // tile_rows
    q_flat = q_blocks.reshape(tiles * tile_rows, width)
    q_tiles = q_docs.reshape(tiles, tile_rows)
    low, high = q_tiles[:, :1], q_tiles[:, -1:]
    key_low, key_high = kv_docs[None, :, 0], kv_docs[None, :, -1]
    needed = (key_low <= high) & (key_high >= low)
    whole = (low == high) & (key_low == key_high)
    flags = jnp.where(needed, jnp.where(whole, 2, 1), 0).astype(jnp.int32).reshape(-1)
    grid_spec = pltpu.PrefetchScalarGridSpec(
        num_scalar_prefetch=1,
        grid=(tiles,),
        in_specs=[
            pl.BlockSpec((tile_rows, width), lambda t, f: (t, 0)),
            pl.BlockSpec((blocks, block_rows, 2 * HD), lambda t, f: (0, 0, 0)),
            pl.BlockSpec((1, 1, group * tile_rows), lambda t, f: (t, 0, 0)),
            pl.BlockSpec((blocks, block_rows, 1), lambda t, f: (0, 0, 0)),
        ],
        out_specs=pl.BlockSpec((tile_rows, width), lambda t, f: (t, 0)),
        scratch_shapes=[
            pltpu.VMEM((1, group * tile_rows), jnp.float32),
            pltpu.VMEM((1, group * tile_rows), jnp.float32),
            pltpu.VMEM((HD, group * tile_rows), jnp.float32),
        ],
    )
    pairs = tiles * tile_rows * group * blocks * block_rows
    out = pl.pallas_call(
        functools.partial(attend_kernel, group=group, blocks=blocks),
        grid_spec=grid_spec,
        out_shape=jax.ShapeDtypeStruct(q_flat.shape, jnp.bfloat16),
        cost_estimate=pl.CostEstimate(
            flops=2 * pairs * HD, bytes_accessed=4 * q_flat.size + 2 * kv_blocks.size, transcendentals=pairs // 2
        ),
        name="attend",
    )(flags, q_flat, kv_blocks, jnp.tile(q_tiles, (1, group))[:, None, :], kv_docs[:, :, None])
    return out.reshape(q_blocks.shape)


def up_kernel(part, col, *refs, tp, slots, slab):
    x_refs, w_ref, out_ref, rows_ref = refs[:tp], refs[tp], refs[tp + 1], refs[tp + 2]

    @pl.when(pl.program_id(0) == 0)
    def _():
        for s in range(slots):
            for j in range(tp):

                @pl.when(part[s] == j)
                def _(s=s, j=j):
                    at = pl.multiple_of(col[s], slab)
                    rows_ref[:, s * slab : (s + 1) * slab] = x_refs[j][:, pl.ds(at, slab)]

    hidden = jnp.dot(rows_ref[...], w_ref[...], preferred_element_type=jnp.float32)
    positive = jnp.maximum(hidden, 0.0)
    out_ref[...] = (positive * positive).astype(jnp.bfloat16)


def up_project(part, col, parts, weight, slots):
    tp = len(parts)
    rows, width = parts[0].shape
    depth, units = weight.shape
    block = min(256, units)
    grid_spec = pltpu.PrefetchScalarGridSpec(
        num_scalar_prefetch=2,
        grid=(units // block,),
        in_specs=[pl.BlockSpec((rows, width), lambda n, a, b: (0, 0))] * tp
        + [pl.BlockSpec((depth, block), lambda n, a, b: (0, n))],
        out_specs=pl.BlockSpec((rows, block), lambda n, a, b: (0, n)),
        scratch_shapes=[pltpu.VMEM((rows, depth), jnp.bfloat16)],
    )
    return pl.pallas_call(
        functools.partial(up_kernel, tp=tp, slots=slots, slab=depth // slots),
        grid_spec=grid_spec,
        out_shape=jax.ShapeDtypeStruct((rows, units), jnp.bfloat16),
        cost_estimate=pl.CostEstimate(
            flops=2 * rows * depth * units, bytes_accessed=2 * depth * (units + rows), transcendentals=0
        ),
    )(part, col, *parts, weight)


def down_kernel(part, col, x_ref, w_ref, *out_refs, slab):
    s = pl.program_id(0)
    result = jnp.dot(x_ref[...], w_ref[...], preferred_element_type=jnp.float32).astype(jnp.bfloat16)
    for j, out_ref in enumerate(out_refs):

        @pl.when(part[s] == j)
        def _(out_ref=out_ref):
            out_ref[:, pl.ds(pl.multiple_of(col[s], slab), slab)] = result


def down_project(part, col, squared, weight, tp, slots):
    rows, units = squared.shape
    slab = weight.shape[1]
    width = slab * slots // tp
    grid_spec = pltpu.PrefetchScalarGridSpec(
        num_scalar_prefetch=2,
        grid=(slots,),
        in_specs=[
            pl.BlockSpec((rows, units), lambda s, a, b: (0, 0)),
            pl.BlockSpec((units, slab), lambda s, a, b: (s, 0)),
        ],
        out_specs=[pl.BlockSpec((rows, width), lambda s, a, b: (0, 0))] * tp,
    )
    return pl.pallas_call(
        functools.partial(down_kernel, slab=slab),
        grid_spec=grid_spec,
        out_shape=[jax.ShapeDtypeStruct((rows, width), jnp.bfloat16)] * tp,
        cost_estimate=pl.CostEstimate(
            flops=2 * rows * units * slab * slots, bytes_accessed=2 * units * (slab * slots + rows), transcendentals=0
        ),
    )(part, col, squared, weight)


def spread(index, bits):
    return sum(((index >> n) & 1) << bit for n, bit in enumerate(bits))


def make_body(sp, tp, near_bits, wide_bits):
    near, wide = 1 << len(near_bits), 1 << len(wide_bits)
    near_mask = [spread(c, near_bits) for c in range(near)]
    wide_mask = [spread(m, wide_bits) for m in range(wide)]
    groups = [[c] for c in range(1, near)]

    def swap(value, mask):
        return lax.ppermute(value, "sp", [(s, s ^ mask) for s in range(sp)])

    def swap_tp(value, j):
        return lax.ppermute(value, "tp", [(t, t ^ j) for t in range(tp)])

    def gather_wide(value):
        if wide != 4:
            return [value] + [swap(value, wide_mask[m]) for m in range(1, wide)]
        high = swap(value, wide_mask[2])
        low = swap(value, wide_mask[1])
        return [value, low, high, swap(high, wide_mask[1])]

    def body(
        queries, keys, values, documents, query_gain, key_gain, residual, out_weight, norm_gain, up_weight, down_weight
    ):
        rows = queries.shape[0]
        key_heads = keys.shape[1] // HD
        group = HQ // KV
        width = residual.shape[1]
        here, t = lax.axis_index("sp"), lax.axis_index("tp")
        own = sum(((here >> bit) & 1) << n for n, bit in enumerate(near_bits))
        split = key_heads % near == 0
        units = up_weight.shape[1] // near
        slab = up_weight.shape[0]
        far = range(1, near)
        places = [(m, c) for cs in [[0]] + groups for m in range(wide) for c in cs]
        slots = len(places)
        spots = jnp.stack([(here ^ (wide_mask[m] ^ near_mask[c])) * slab for m, c in places]).astype(jnp.int32)
        part = (spots // width) ^ t.astype(jnp.int32)
        col = spots % width

        def units_of(weight, c, axis):
            return lax.dynamic_slice_in_dim(weight, (own ^ c) * units, units, axis)

        def gather_units(weight, axis):
            pieces = {c: swap(units_of(weight, c, axis), near_mask[c]) for c in far}
            found = gather_wide(units_of(weight, 0, axis))
            for cs in groups:
                stacked = pieces[cs[0]] if len(cs) == 1 else jnp.concatenate([pieces[c] for c in cs])
                found += gather_wide(stacked)
            return jnp.concatenate(found)

        up_whole = gather_units(up_weight, 1)
        down_whole = gather_units(down_weight, 0)

        docs_near = jnp.stack([documents] + [swap(documents, near_mask[c]) for c in far])
        docs_all = jnp.concatenate([docs_near] + [swap(docs_near, wide_mask[m]) for m in range(1, wide)])

        positions = here * rows + jnp.arange(rows, dtype=jnp.int32)
        queries_rot = grid_rotary(
            head_norm(queries.reshape(rows, key_heads * group, HD), query_gain), positions
        ).astype(jnp.bfloat16)
        keys_rot = grid_rotary(head_norm(keys.reshape(rows, key_heads, HD), key_gain), positions).astype(jnp.bfloat16)
        parts = near if split else 1
        heads = key_heads // parts
        q_width = heads * group * HD
        packed = jnp.concatenate(
            [
                queries_rot.reshape(rows, parts, q_width),
                keys_rot.reshape(rows, parts, heads * HD),
                values.reshape(rows, parts, heads * HD),
            ],
            axis=-1,
        )
        packed = jnp.transpose(packed, (1, 0, 2))
        if split:
            taken = [lax.dynamic_index_in_dim(packed, own ^ c, 0, keepdims=False) for c in range(near)]
            taken = [taken[0]] + [swap(taken[c], near_mask[c]) for c in far]
            q_blocks = jnp.stack([piece[:, :q_width] for piece in taken])
            kv_own = jnp.concatenate([piece[:, q_width:] for piece in taken])
            q_docs = docs_near
        else:
            q_blocks = packed[:, :, :q_width]
            kv_mine = packed[0, :, q_width:]
            kv_own = jnp.concatenate([kv_mine] + [swap(kv_mine, near_mask[c]) for c in far])
            q_docs = documents[None]
        kv_all = jnp.concatenate(gather_wide(kv_own)).reshape(near * wide, rows, -1)

        attended = []
        for h in range(heads):
            q_head = q_blocks[:, :, h * group * HD : (h + 1) * group * HD]
            kv_head = kv_all
            if heads > 1:
                kv_head = jnp.concatenate(
                    [kv_all[:, :, h * HD : (h + 1) * HD], kv_all[:, :, (heads + h) * HD : (heads + h + 1) * HD]], -1
                )
            attended.append(attend(q_head, kv_head, q_docs, docs_all, group))
        attended = attended[0] if heads == 1 else jnp.concatenate(attended, -1)
        if split:
            merged = jnp.zeros((rows, near * q_width), jnp.bfloat16)
            for c in range(near):
                piece = attended[c] if c == 0 else swap(attended[c], near_mask[c])
                merged = lax.dynamic_update_slice_in_dim(merged, piece, (own ^ c) * q_width, 1)
            attended = merged
        else:
            attended = attended[0]

        partial_out = jnp.dot(attended, out_weight, preferred_element_type=jnp.float32).astype(jnp.bfloat16)
        stream = residual.astype(jnp.float32)
        for j in range(tp):
            piece = lax.dynamic_slice_in_dim(partial_out, (t ^ j) * width, width, 1)
            piece = piece if j == 0 else swap_tp(piece, j)
            stream = stream + piece.astype(jnp.float32)
        squares = jnp.sum(stream * stream, axis=-1)
        total_squares = squares
        for j in range(1, tp):
            total_squares = total_squares + swap_tp(squares, j)
        gain_here = lax.dynamic_slice_in_dim(norm_gain, t * width, width, 0)
        normed = stream * lax.rsqrt(total_squares / (width * tp) + norm_eps)[:, None]
        normed = (normed * gain_here).astype(jnp.bfloat16)

        chunks = [normed] * near
        for c in far:
            low = c & -c
            via = chunks[c ^ low] if c != low else normed
            chunks[c] = swap(via, near_mask[low])
        squared = []
        for c in range(near):
            chunk_parts = [chunks[c]] + [swap_tp(chunks[c], j) for j in range(1, tp)]
            squared.append(up_project(part, col, chunk_parts, up_whole, slots))
        feed = [None] * near
        for c in list(far)[::-1] + [0]:
            pieces = down_project(part, col, squared[c], down_whole, tp, slots)
            total = pieces[0].astype(jnp.float32)
            for j in range(1, tp):
                total = total + swap_tp(pieces[j], j).astype(jnp.float32)
            feed[c] = total
        for c in list(far)[::-1]:
            low = c & -c
            arrived = swap(feed[c].astype(jnp.bfloat16), near_mask[low])
            feed[c ^ low] = feed[c ^ low] + arrived.astype(jnp.float32)
        return (stream + feed[0]).astype(jnp.bfloat16)

    return body


def solution(mesh):
    sp, tp = mesh.shape["sp"], mesh.shape["tp"]
    bits = range(sp.bit_length() - 1)
    near_bits, wide_bits = bits[0::2], bits[1::2]
    in_specs = (
        P("sp", "tp"),
        P("sp", "tp"),
        P("sp", "tp"),
        P("sp"),
        P(),
        P(),
        P("sp", "tp"),
        P("tp", None),
        P(),
        P("sp", "tp"),
        P("tp", "sp"),
    )
    return jax.shard_map(
        make_body(sp, tp, near_bits, wide_bits), mesh=mesh, in_specs=in_specs, out_specs=P("sp", "tp"), check_vma=False
    )
```

```python
import functools
import jax
import jax.numpy as jnp
from jax import lax
from jax.experimental import pallas as pl
from jax.experimental.pallas import tpu as pltpu
from jax.sharding import PartitionSpec as P


HQ = 16
KV = 8
HD = 128
GRID_W = 64

norm_eps = 1e-06
rope_base = 10000.0
masked_score = -1e30
log2_e = 1.4426950408889634


def head_norm(heads_in, gain):
    values32 = heads_in.astype(jnp.float32)
    scaled = values32 * lax.rsqrt(jnp.mean(values32 * values32, axis=-1, keepdims=True) + norm_eps)
    return scaled * gain


def rotate_half(heads_in, position):
    quarter = heads_in.shape[-1] // 2
    inverse_freq = rope_base ** (-jnp.arange(quarter, dtype=jnp.float32) / quarter)
    angles = position[:, None] * inverse_freq[None, :]
    cosine_part = jnp.cos(angles)[:, None, :]
    sine_part = jnp.sin(angles)[:, None, :]
    leading = heads_in[..., :quarter]
    trailing = heads_in[..., quarter:]
    return jnp.concatenate(
        [
            leading * cosine_part - trailing * sine_part,
            leading * sine_part + trailing * cosine_part,
        ],
        axis=-1,
    )


def grid_rotary(heads_in, positions):
    half_width = heads_in.shape[-1] // 2
    grid_row = (positions // GRID_W).astype(jnp.float32)
    grid_col = (positions % GRID_W).astype(jnp.float32)
    return jnp.concatenate(
        [
            rotate_half(heads_in[..., :half_width], grid_row),
            rotate_half(heads_in[..., half_width:], grid_col),
        ],
        axis=-1,
    )


def attend_kernel(flags, q_ref, kv_ref, qdoc_ref, kdoc_ref, out_ref, max_ref, sum_ref, acc_ref, *, group, blocks):
    tile = pl.program_id(0)
    tokens = q_ref.shape[0]
    factor = log2_e * HD ** (-0.5)
    rows = jnp.concatenate([q_ref[:, g * HD : (g + 1) * HD] for g in range(group)], axis=0)
    max_ref[...] = jnp.full(max_ref.shape, masked_score, jnp.float32)
    sum_ref[...] = jnp.zeros(sum_ref.shape, jnp.float32)
    acc_ref[...] = jnp.zeros(acc_ref.shape, jnp.float32)

    def block_step(block, masked):
        scores = lax.dot_general(
            kv_ref[block, :, :HD], rows, (((1,), (1,)), ((), ())), preferred_element_type=jnp.float32
        )
        if masked:
            same = kdoc_ref[block] == qdoc_ref[0]
            scores = jnp.where(same, scores, masked_score)
        old_max = max_ref[...]
        new_max = jnp.maximum(old_max, jnp.max(scores, axis=0, keepdims=True))
        alpha = jnp.exp2((old_max - new_max) * factor)
        probs = jnp.exp2((scores - new_max) * factor)
        if masked:
            probs = jnp.where(same, probs, 0.0)
        sum_ref[...] = sum_ref[...] * alpha + jnp.sum(probs, axis=0, keepdims=True)
        acc_ref[...] = acc_ref[...] * alpha + lax.dot_general(
            kv_ref[block, :, HD:],
            probs.astype(jnp.bfloat16),
            (((0,), (0,)), ((), ())),
            preferred_element_type=jnp.float32,
        )
        max_ref[...] = new_max

    def loop_body(block, carry):
        kind = flags[tile * blocks + block]

        @pl.when(kind == 1)
        def _():
            block_step(block, True)

        @pl.when(kind == 2)
        def _():
            block_step(block, False)

        return carry

    lax.fori_loop(0, blocks, loop_body, 0)
    result = jnp.transpose(acc_ref[...] / sum_ref[...]).astype(jnp.bfloat16)
    for g in range(group):
        out_ref[:, g * HD : (g + 1) * HD] = result[g * tokens : (g + 1) * tokens]


def attend(q_blocks, kv_blocks, q_docs, kv_docs, group):
    q_count, rows, width = q_blocks.shape
    blocks, block_rows, _ = kv_blocks.shape
    tile_rows = min(256, rows)
    tiles = q_count * rows // tile_rows
    q_flat = q_blocks.reshape(tiles * tile_rows, width)
    q_tiles = q_docs.reshape(tiles, tile_rows)
    low, high = q_tiles[:, :1], q_tiles[:, -1:]
    key_low, key_high = kv_docs[None, :, 0], kv_docs[None, :, -1]
    needed = (key_low <= high) & (key_high >= low)
    whole = (low == high) & (key_low == key_high)
    flags = jnp.where(needed, jnp.where(whole, 2, 1), 0).astype(jnp.int32).reshape(-1)
    grid_spec = pltpu.PrefetchScalarGridSpec(
        num_scalar_prefetch=1,
        grid=(tiles,),
        in_specs=[
            pl.BlockSpec((tile_rows, width), lambda t, f: (t, 0)),
            pl.BlockSpec((blocks, block_rows, 2 * HD), lambda t, f: (0, 0, 0)),
            pl.BlockSpec((1, 1, group * tile_rows), lambda t, f: (t, 0, 0)),
            pl.BlockSpec((blocks, block_rows, 1), lambda t, f: (0, 0, 0)),
        ],
        out_specs=pl.BlockSpec((tile_rows, width), lambda t, f: (t, 0)),
        scratch_shapes=[
            pltpu.VMEM((1, group * tile_rows), jnp.float32),
            pltpu.VMEM((1, group * tile_rows), jnp.float32),
            pltpu.VMEM((HD, group * tile_rows), jnp.float32),
        ],
    )
    pairs = tiles * tile_rows * group * blocks * block_rows
    out = pl.pallas_call(
        functools.partial(attend_kernel, group=group, blocks=blocks),
        grid_spec=grid_spec,
        out_shape=jax.ShapeDtypeStruct(q_flat.shape, jnp.bfloat16),
        cost_estimate=pl.CostEstimate(
            flops=2 * pairs * HD, bytes_accessed=4 * q_flat.size + 2 * kv_blocks.size, transcendentals=pairs // 2
        ),
        name="attend",
    )(flags, q_flat, kv_blocks, jnp.tile(q_tiles, (1, group))[:, None, :], kv_docs[:, :, None])
    return out.reshape(q_blocks.shape)


def up_kernel(part, col, *refs, tp, count, slots, slab):
    x_refs, w_ref, out_ref, rows_ref = refs[: count * tp], refs[count * tp], refs[count * tp + 1], refs[count * tp + 2]
    rows = x_refs[0].shape[0]

    @pl.when(pl.program_id(0) == 0)
    def _():
        for s in range(slots):
            for j in range(tp):

                @pl.when(part[s] == j)
                def _(s=s, j=j):
                    at = pl.multiple_of(col[s], slab)
                    for n in range(count):
                        rows_ref[n * rows : (n + 1) * rows, s * slab : (s + 1) * slab] = x_refs[n * tp + j][
                            :, pl.ds(at, slab)
                        ]

    hidden = jnp.dot(rows_ref[...], w_ref[...], preferred_element_type=jnp.float32)
    positive = jnp.maximum(hidden, 0.0)
    out_ref[...] = (positive * positive).astype(jnp.bfloat16)


def up_project(part, col, chunks, weight, slots):
    count, tp = len(chunks), len(chunks[0])
    rows, width = chunks[0][0].shape
    depth, units = weight.shape
    block = min(256, units)
    grid_spec = pltpu.PrefetchScalarGridSpec(
        num_scalar_prefetch=2,
        grid=(units // block,),
        in_specs=[pl.BlockSpec((rows, width), lambda n, a, b: (0, 0))] * (count * tp)
        + [pl.BlockSpec((depth, block), lambda n, a, b: (0, n))],
        out_specs=pl.BlockSpec((count * rows, block), lambda n, a, b: (0, n)),
        scratch_shapes=[pltpu.VMEM((count * rows, depth), jnp.bfloat16)],
    )
    return pl.pallas_call(
        functools.partial(up_kernel, tp=tp, count=count, slots=slots, slab=depth // slots),
        grid_spec=grid_spec,
        out_shape=jax.ShapeDtypeStruct((count * rows, units), jnp.bfloat16),
        cost_estimate=pl.CostEstimate(
            flops=2 * count * rows * depth * units,
            bytes_accessed=2 * depth * (units + count * rows),
            transcendentals=0,
        ),
    )(part, col, *[piece for chunk in chunks for piece in chunk], weight)


def down_kernel(part, col, x_ref, w_ref, *refs):
    out_ref = refs[-1]
    out_ref[0] = jnp.dot(x_ref[...], w_ref[...], preferred_element_type=jnp.float32).astype(jnp.bfloat16)


def down_project(part, col, squared, weight, tp, slots, first, into):
    rows, units = squared.shape
    slab = weight.shape[1]
    count = weight.shape[0] // units
    width = slab * slots // tp
    grid_spec = pltpu.PrefetchScalarGridSpec(
        num_scalar_prefetch=2,
        grid=(count,),
        in_specs=[
            pl.BlockSpec((rows, units), lambda s, a, b: (0, 0)),
            pl.BlockSpec((units, slab), lambda s, a, b: (s, 0)),
        ]
        + ([] if into is None else [pl.BlockSpec(memory_space=pl.ANY)]),
        out_specs=pl.BlockSpec((1, rows, slab), lambda s, a, b: (a[first + s], 0, b[first + s] // slab)),
    )
    return pl.pallas_call(
        down_kernel,
        grid_spec=grid_spec,
        out_shape=jax.ShapeDtypeStruct((tp, rows, width), jnp.bfloat16),
        input_output_aliases={} if into is None else {4: 0},
        cost_estimate=pl.CostEstimate(
            flops=2 * rows * units * slab * count,
            bytes_accessed=2 * units * (slab * count + rows),
            transcendentals=0,
        ),
    )(part, col, squared, weight, *([] if into is None else [into]))


def part_sum(pieces, offset, start, stop):
    return sum(piece[offset + start : offset + stop].astype(jnp.float32) for piece in pieces)


def spread(index, bits):
    return sum(((index >> n) & 1) << bit for n, bit in enumerate(bits))


def make_body(sp, tp, near_bits, wide_bits):
    near, wide = 1 << len(near_bits), 1 << len(wide_bits)
    near_mask = [spread(c, near_bits) for c in range(near)]
    wide_mask = [spread(m, wide_bits) for m in range(wide)]
    groups = [[c] for c in range(1, near)]

    def swap(value, mask):
        return lax.ppermute(value, "sp", [(s, s ^ mask) for s in range(sp)])

    def swap_tp(value, j):
        return lax.ppermute(value, "tp", [(t, t ^ j) for t in range(tp)])

    def gather_wide(value):
        if wide != 4:
            return [value] + [swap(value, wide_mask[m]) for m in range(1, wide)]
        high = swap(value, wide_mask[2])
        low = swap(value, wide_mask[1])
        return [value, low, high, swap(high, wide_mask[1])]

    def body(
        queries, keys, values, documents, query_gain, key_gain, residual, out_weight, norm_gain, up_weight, down_weight
    ):
        rows = queries.shape[0]
        key_heads = keys.shape[1] // HD
        group = HQ // KV
        width = residual.shape[1]
        here, t = lax.axis_index("sp"), lax.axis_index("tp")
        own = sum(((here >> bit) & 1) << n for n, bit in enumerate(near_bits))
        split = key_heads % near == 0
        units = up_weight.shape[1] // near
        slab = up_weight.shape[0]
        far = range(1, near)
        places = [(m, c) for cs in [[0]] + groups for m in range(wide) for c in cs]
        slots = len(places)
        spots = jnp.stack([(here ^ (wide_mask[m] ^ near_mask[c])) * slab for m, c in places]).astype(jnp.int32)
        part = (spots // width) ^ t.astype(jnp.int32)
        col = spots % width

        def units_of(weight, c, axis):
            return lax.dynamic_slice_in_dim(weight, (own ^ c) * units, units, axis)

        def gather_units(weight, axis):
            pieces = {c: swap(units_of(weight, c, axis), near_mask[c]) for c in far}
            found = gather_wide(units_of(weight, 0, axis))
            for cs in groups:
                stacked = pieces[cs[0]] if len(cs) == 1 else jnp.concatenate([pieces[c] for c in cs])
                found += gather_wide(stacked)
            return found

        up_whole = jnp.concatenate(gather_units(up_weight, 1))
        down_found = gather_units(down_weight, 0)
        late = slots - 2 * wide
        down_early, down_late = jnp.concatenate(down_found[:late]), jnp.concatenate(down_found[late:])

        docs_near = jnp.stack([documents] + [swap(documents, near_mask[c]) for c in far])
        docs_all = jnp.concatenate([docs_near] + [swap(docs_near, wide_mask[m]) for m in range(1, wide)])

        positions = here * rows + jnp.arange(rows, dtype=jnp.int32)
        queries_rot = grid_rotary(
            head_norm(queries.reshape(rows, key_heads * group, HD), query_gain), positions
        ).astype(jnp.bfloat16)
        keys_rot = grid_rotary(head_norm(keys.reshape(rows, key_heads, HD), key_gain), positions).astype(jnp.bfloat16)
        parts = near if split else 1
        heads = key_heads // parts
        q_width = heads * group * HD
        packed = jnp.concatenate(
            [
                queries_rot.reshape(rows, parts, q_width),
                keys_rot.reshape(rows, parts, heads * HD),
                values.reshape(rows, parts, heads * HD),
            ],
            axis=-1,
        )
        packed = jnp.transpose(packed, (1, 0, 2))
        if split:
            taken = [lax.dynamic_index_in_dim(packed, own ^ c, 0, keepdims=False) for c in range(near)]
            taken = [taken[0]] + [swap(taken[c], near_mask[c]) for c in far]
            q_blocks = jnp.stack([piece[:, :q_width] for piece in taken])
            kv_own = jnp.concatenate([piece[:, q_width:] for piece in taken])
            q_docs = docs_near
        else:
            q_blocks = packed[:, :, :q_width]
            kv_mine = packed[0, :, q_width:]
            kv_own = jnp.concatenate([kv_mine] + [swap(kv_mine, near_mask[c]) for c in far])
            q_docs = documents[None]
        kv_all = jnp.concatenate(gather_wide(kv_own)).reshape(near * wide, rows, -1)

        attended = []
        for h in range(heads):
            q_head = q_blocks[:, :, h * group * HD : (h + 1) * group * HD]
            kv_head = kv_all
            if heads > 1:
                kv_head = jnp.concatenate(
                    [kv_all[:, :, h * HD : (h + 1) * HD], kv_all[:, :, (heads + h) * HD : (heads + h + 1) * HD]], -1
                )
            attended.append(attend(q_head, kv_head, q_docs, docs_all, group))
        attended = attended[0] if heads == 1 else jnp.concatenate(attended, -1)
        if split:
            merged = jnp.zeros((rows, near * q_width), jnp.bfloat16)
            for c in range(near):
                piece = attended[c] if c == 0 else swap(attended[c], near_mask[c])
                merged = lax.dynamic_update_slice_in_dim(merged, piece, (own ^ c) * q_width, 1)
            attended = merged
        else:
            attended = attended[0]

        partial_out = jnp.dot(attended, out_weight, preferred_element_type=jnp.float32).astype(jnp.bfloat16)
        stream = residual.astype(jnp.float32)
        for j in range(tp):
            piece = lax.dynamic_slice_in_dim(partial_out, (t ^ j) * width, width, 1)
            piece = piece if j == 0 else swap_tp(piece, j)
            stream = stream + piece.astype(jnp.float32)
        squares = jnp.sum(stream * stream, axis=-1)
        total_squares = squares
        for j in range(1, tp):
            total_squares = total_squares + swap_tp(squares, j)
        gain_here = lax.dynamic_slice_in_dim(norm_gain, t * width, width, 0)
        normed = stream * lax.rsqrt(total_squares / (width * tp) + norm_eps)[:, None]
        normed = (normed * gain_here).astype(jnp.bfloat16)

        chunks = [normed] * near
        for c in far:
            low = c & -c
            via = chunks[c ^ low] if c != low else normed
            chunks[c] = swap(via, near_mask[low])
        parts_of = [[chunks[c]] + [swap_tp(chunks[c], j) for j in range(1, tp)] for c in range(near)]
        feed = [None] * near
        for c in range(0, near, 2):
            squared = up_project(part, col, parts_of[c : c + 2], up_whole, slots)
            product = down_project(part, col, squared, down_early, tp, slots, 0, None)
            product = down_project(part, col, squared, down_late, tp, slots, late, product)
            heard = [product[0]] + [swap_tp(product[j], j) for j in range(1, tp)]
            feed[c] = functools.partial(part_sum, heard, 0)
            feed[c + 1] = functools.partial(part_sum, heard, rows)
        if near == 4:
            half, low, high = rows // 2, near_mask[1], near_mask[2]

            def send(value, mask):
                return swap(value.astype(jnp.bfloat16), mask).astype(jnp.float32)

            def low_bits(value):
                return value.astype(jnp.bfloat16)

            three_a, three_b, two_b, two_a = lax.optimization_barrier(
                (low_bits(feed[3](0, half)), low_bits(feed[3](half, rows)), low_bits(feed[2](half, rows)), feed[2](0, half))
            )
            low_3, high_3, high_2 = send(three_a, low), send(three_b, high), send(two_b, high)
            one_a, one_b, own_a, own_b = lax.optimization_barrier(
                (low_bits(feed[1](0, half)), feed[1](half, rows), feed[0](0, half), feed[0](half, rows))
            )
            low_1 = send(one_a, low)
            mixed_a = low_bits(two_a + low_3)
            high_a = send(mixed_a, high)
            mixed_b = low_bits(one_b + high_3)
            low_b = send(mixed_b, low)
            top = stream[:half] + (own_a + low_1 + high_a)
            bottom = stream[half:] + (own_b + high_2 + low_b)
            return jnp.concatenate([top.astype(jnp.bfloat16), bottom.astype(jnp.bfloat16)])
        feed = [one(0, rows) for one in feed]
        for c in list(far)[::-1]:
            bit = c & -c
            arrived = swap(feed[c].astype(jnp.bfloat16), near_mask[bit])
            feed[c ^ bit] = feed[c ^ bit] + arrived.astype(jnp.float32)
        return (stream + feed[0]).astype(jnp.bfloat16)

    return body


def solution(mesh):
    sp, tp = mesh.shape["sp"], mesh.shape["tp"]
    bits = range(sp.bit_length() - 1)
    near_bits, wide_bits = bits[0::2], bits[1::2]
    in_specs = (
        P("sp", "tp"),
        P("sp", "tp"),
        P("sp", "tp"),
        P("sp"),
        P(),
        P(),
        P("sp", "tp"),
        P("tp", None),
        P(),
        P("sp", "tp"),
        P("tp", "sp"),
    )
    return jax.shard_map(
        make_body(sp, tp, near_bits, wide_bits), mesh=mesh, in_specs=in_specs, out_specs=P("sp", "tp"), check_vma=False
    )
```
